32 devices in a mesh: sp: 16 (over z, y, x), tp: 2 (over core).
Axes of the slice: x: 2, y: 2, z: 4, core: 2. Of those that a mesh axis runs over, the one named last changes fastest.
Arguments:
- tokens: bfloat16 [4096, 2048], P('sp', 'tp'), may hold values from -6 to 6
- norm_gain: float32 [2048], replicated, may hold values from 0.1 to 1.9
- recur_query: bfloat16 [2048, 1024], P(None, 'tp'), may hold values from -0.125 to 0.125
- recur_forget: bfloat16 [2048, 1024], P(None, 'tp'), may hold values from -0.125 to 0.125
- recur_value: bfloat16 [2048, 1024], P(None, 'tp'), may hold values from -0.125 to 0.125
- gate_floor: float32 [1024], P('tp'), may hold values from 0.5 to 1
- extra_decay: float32 [4096, 8], P('sp', 'tp'), may hold values from 0 to 2
- start_state: float32 [8, 128, 128], P('tp'), may hold values from -0.125 to 0.125
- recur_gain: float32 [1024], P('tp'), may hold values from 0.1 to 1.9
- attend_query: bfloat16 [2048, 1024], P(None, 'tp')
- attend_key: bfloat16 [2048, 1024], P(None, 'tp')
- attend_value: bfloat16 [2048, 1024], P(None, 'tp'), may hold values from -0.125 to 0.125
- gate_cache: float32 [4096, 16], P(None, 'tp'), may hold values from -4096 to 0, as said below
- attend_gain: float32 [1024], P('tp'), may hold values from 0.1 to 1.9
- recur_output: bfloat16 [1024, 2048], P(None, 'tp'), may hold values from -0.1875 to 0.1875
- attend_output: bfloat16 [1024, 2048], P(None, 'tp'), may hold values from -0.1875 to 0.1875
Outputs:
- layer_output: bfloat16 [4096, 2048], P('sp', 'tp')
The draws below stay inside these ranges and needn't reach their ends.
Inputs may be any that keep to these rules, and one draw needn't show every extreme that they name: `gate_cache`: never rising along positions.
All inputs are finite; a program needn't handle non-finite values.
Results may differ from the reference program's by a relative error of at most 0.018.
Values may be sent and summed in bfloat16 or wider, within the bound.
A program may use at most 64 MiB of HBM per device.

```python
import jax
import jax.numpy as jnp
from jax import lax

D = 2048
RECUR_HEAD_COUNT = 8
KD = 128
VD = 128
FORGET_HEAD_COUNT = 16
FD = 64
TOK_DEV = 256
TOKEN_COUNT = 4096


def fast_heads(key, total_amount):
    order = jax.random.permutation(key, total_amount)
    return order < total_amount // 2


def spike_rates(key, total_amount):
    blocks = TOKEN_COUNT // TOK_DEV
    factor = jnp.exp(jax.random.uniform(jax.random.fold_in(key, 1), (blocks, 1, total_amount), jnp.float32, 0.0, jnp.log(4.0)))
    jitter = jax.random.uniform(jax.random.fold_in(key, 2), (blocks, TOK_DEV, total_amount), jnp.float32, 0.5, 1.5)
    steady_value = 0.3 / TOKEN_COUNT * factor * jitter
    spot_index = jax.random.randint(jax.random.fold_in(key, 3), (2, total_amount), 0, TOKEN_COUNT)
    block_sizes = jax.random.uniform(jax.random.fold_in(key, 4), (2, total_amount), jnp.float32, 0.22, 0.69)
    place_index = jnp.arange(TOKEN_COUNT)[:, None, None]
    spike_list = jnp.sum(jnp.where(place_index == spot_index[None], block_sizes[None], 0.0), axis=1)
    return steady_value.reshape(TOKEN_COUNT, total_amount) + spike_list


def draw_gate_floor(key, part):
    quick = fast_heads(jax.random.fold_in(key, 1), RECUR_HEAD_COUNT)
    slow_gap = jnp.exp(jax.random.uniform(jax.random.fold_in(key, 2), (RECUR_HEAD_COUNT, KD), jnp.float32, jnp.log(0.2), jnp.log(0.8))) / TOKEN_COUNT
    quick_floor = jax.random.uniform(jax.random.fold_in(key, 3), (RECUR_HEAD_COUNT, KD), jnp.float32, 0.8, 0.95)
    floors = jnp.where(quick[:, None], quick_floor, 1.0 - slow_gap)
    return floors.reshape(RECUR_HEAD_COUNT * KD)


def draw_extra_decay(key, part):
    return spike_rates(jax.random.fold_in(key, 5), RECUR_HEAD_COUNT)


def draw_gate_cache(key, part):
    gradual_steps = spike_rates(jax.random.fold_in(key, 6), FORGET_HEAD_COUNT)
    quick = fast_heads(jax.random.fold_in(key, 7), FORGET_HEAD_COUNT)
    blocks = TOKEN_COUNT // TOK_DEV
    factor = jnp.exp(jax.random.uniform(jax.random.fold_in(key, 8), (blocks, 1, FORGET_HEAD_COUNT), jnp.float32, 0.0, jnp.log(4.0)))
    rates = jax.random.uniform(jax.random.fold_in(key, 9), (blocks, TOK_DEV, FORGET_HEAD_COUNT), jnp.float32, 0.005, 0.02)
    quick_steps = (rates * factor).reshape(TOKEN_COUNT, FORGET_HEAD_COUNT)
    steps_all = jnp.where(quick[None, :], quick_steps, gradual_steps)
    return -jnp.cumsum(steps_all, axis=0)


def key_base(key):
    return jax.random.normal(jax.random.fold_in(key, 21), (D, FORGET_HEAD_COUNT * FD), jnp.float32) / jnp.sqrt(1.0 * D)


def draw_attend_key(key, part):
    return key_base(key).astype(jnp.bfloat16)


def draw_attend_query(key, part):
    fresh = jax.random.normal(jax.random.fold_in(key, 22), (D, FORGET_HEAD_COUNT * FD), jnp.float32) / jnp.sqrt(1.0 * D)
    return fresh.astype(jnp.bfloat16)


def level_of(rng, shape, split, least, high):
    factor_of = 1.0
    for position, blocks in split:
        steps = jax.random.uniform(jax.random.fold_in(jax.random.fold_in(rng, 6), position), (blocks,), jnp.float32, least / len(split), high / len(split))
        factor_of = factor_of * jnp.repeat(jnp.exp(steps), shape[position] // blocks).reshape((-1,) + (1,) * (len(shape) - 1 - position))
    return factor_of


def centred(key, extent, deviation, limit, split=(), held_as=jnp.bfloat16):
    result = jax.random.normal(key, extent, jnp.float32) * deviation
    if len(split) > 0:
        result = level_of(key, extent, split, -0.22, 0.18) * result
    return jnp.clip(result, min=-limit, max=limit).astype(held_as)


def setup_inputs(seed: int = 0) -> dict:
    keys = jax.random.split(jax.random.key(seed), 17)
    tokens = centred(keys[0], (TOKEN_COUNT, D), 1.0, 6.0, ((0, 16), (1, 2)))
    norm_gain = jnp.clip(1.0 + 0.18 * jax.random.normal(keys[1], (D,), jnp.float32), 0.1, 1.9)
    recur_query = centred(keys[2], (D, RECUR_HEAD_COUNT * KD), D ** -0.5, 0.125, ((1, 2),))
    recur_forget = centred(keys[3], (D, RECUR_HEAD_COUNT * KD), D ** -0.5, 0.125, ((1, 2),))
    recur_value = centred(keys[4], (D, RECUR_HEAD_COUNT * VD), D ** -0.5, 0.125, ((1, 2),))
    gate_floor = draw_gate_floor(jax.random.fold_in(keys[16], 71), 0)
    extra_decay = draw_extra_decay(jax.random.fold_in(keys[16], 71), 0)
    start_state = centred(keys[7], (RECUR_HEAD_COUNT, KD, VD), (0.5 / TOKEN_COUNT ** 0.5), 0.125, ((0, 2),), jnp.float32)
    recur_gain = jnp.clip(1.0 + 0.18 * jax.random.normal(keys[8], (RECUR_HEAD_COUNT * VD,), jnp.float32), 0.1, 1.9)
    attend_query = draw_attend_query(jax.random.fold_in(keys[16], 71), 0)
    attend_key = draw_attend_key(jax.random.fold_in(keys[16], 71), 0)
    attend_value = centred(keys[11], (D, FORGET_HEAD_COUNT * FD), D ** -0.5, 0.125, ((1, 2),))
    gate_cache = draw_gate_cache(jax.random.fold_in(keys[16], 71), 0)
    attend_gain = jnp.clip(1.0 + 0.18 * jax.random.normal(keys[13], (FORGET_HEAD_COUNT * FD,), jnp.float32), 0.1, 1.9)
    recur_output = centred(keys[14], (RECUR_HEAD_COUNT * VD, D), (RECUR_HEAD_COUNT * VD) ** -0.5, 0.1875, ((1, 2),))
    attend_output = centred(keys[15], (FORGET_HEAD_COUNT * FD, D), (FORGET_HEAD_COUNT * FD) ** -0.5, 0.1875, ((1, 2),))
    return {"tokens": tokens, "norm_gain": norm_gain, "recur_query": recur_query, "recur_forget": recur_forget, "recur_value": recur_value, "gate_floor": gate_floor, "extra_decay": extra_decay, "start_state": start_state, "recur_gain": recur_gain, "attend_query": attend_query, "attend_key": attend_key, "attend_value": attend_value, "gate_cache": gate_cache, "attend_gain": attend_gain, "recur_output": recur_output, "attend_output": attend_output}


EPSILON = 1e-06
TOP_PRECISION = lax.Precision.HIGHEST

def head_norm(per_head, head_gain):
    normed = per_head * lax.rsqrt(lax.optimization_barrier(jnp.mean(per_head * per_head, axis=-1, keepdims=True)) + EPSILON)
    return normed.reshape(per_head.shape[0], -1) * head_gain

def recurrence(query_rows, decays, inflow, values, initial):
    span_len = 64
    blocks = query_rows.shape[0] // span_len

    def to_blocks(tensor):
        return tensor.reshape(blocks, span_len, tensor.shape[1], tensor.shape[2])
    causal = jnp.tril(jnp.ones((span_len, span_len), dtype=bool))[:, :, None, None]

    def advance(carried_state, pieces):
        query_block, g_block, k_block, value_block = pieces
        running_total = jnp.cumsum(g_block, axis=0)
        offsets = jnp.where(causal, running_total[:, None] - running_total[None, :], -jnp.inf)
        mixing = jnp.einsum('thk,shk,tshk->hts', query_block, k_block, jnp.exp(offsets), precision=TOP_PRECISION)
        final_result = jnp.einsum('hts,shv->thv', mixing, value_block, precision=TOP_PRECISION)
        final_result = final_result + jnp.einsum('dzc,zcu->dzu', query_block * jnp.exp(running_total), carried_state, precision=TOP_PRECISION)
        ending_state = running_total[-1]
        weighted_values = k_block * jnp.exp(ending_state[None] - running_total)
        carried_state = jnp.exp(ending_state)[..., None] * carried_state + jnp.einsum('cun,cub->unb', weighted_values, value_block, precision=TOP_PRECISION)
        return (carried_state, final_result)
    _, results = lax.scan(advance, initial, (to_blocks(query_rows), to_blocks(decays), to_blocks(inflow), to_blocks(values)))
    return results.reshape(query_rows.shape[0], query_rows.shape[1], values.shape[2])

def attention(query_rows, key_rows, value_rows, gate_sums):
    length = query_rows.shape[0]
    height = min(256, length)
    blocks = length // height
    scaling = query_rows.shape[2] ** (-0.5)
    key_index = jnp.arange(length)
    keys_wide = key_rows.astype(jnp.float32)
    values_wide = value_rows.astype(jnp.float32)

    def one_block(number):
        first_row = number * height
        query_block = lax.dynamic_slice_in_dim(query_rows, first_row, height, 0).astype(jnp.float32)
        g_block = lax.dynamic_slice_in_dim(gate_sums, first_row, height, 0)
        scores = jnp.einsum('qhd,khd->hqk', query_block, keys_wide) * scaling
        scores = scores + g_block.T[:, :, None] - gate_sums.T[:, None, :]
        query_index = first_row + jnp.arange(height)
        allowed = key_index[None, :] <= query_index[:, None]
        scores = jnp.where(allowed[None], scores, -jnp.inf)
        maxima = lax.optimization_barrier(jnp.max(scores, axis=-1, keepdims=True))
        weights = jnp.exp(scores - maxima)
        totals = lax.optimization_barrier(jnp.sum(weights, axis=-1))
        rounded = lax.optimization_barrier(weights.astype(jnp.bfloat16)).astype(jnp.float32)
        summed = jnp.einsum('hqk,khd->qhd', rounded, values_wide)
        return summed / totals.T[:, :, None]
    results = lax.map(one_block, jnp.arange(blocks))
    return results.reshape(length, query_rows.shape[1], query_rows.shape[2])

def reference(tokens, norm_gain, recur_query, recur_forget, recur_value, gate_floor, extra_decay, start_state, recur_gain, attend_query, attend_key, attend_value, gate_cache, attend_gain, recur_output, attend_output):
    length = tokens.shape[0]
    wide = tokens.astype(jnp.float32)
    inverse = lax.rsqrt(lax.optimization_barrier(jnp.mean(wide * wide, axis=1, keepdims=True)) + EPSILON)
    scaled = (wide * norm_gain).astype(jnp.bfloat16)

    def project(weight):
        return (jnp.dot(scaled, weight, preferred_element_type=jnp.float32) * inverse).astype(jnp.bfloat16)
    rec_heads = start_state.shape[0]
    query_rows = project(recur_query).astype(jnp.float32).reshape(length, rec_heads, -1)
    forget_pre = project(recur_forget).astype(jnp.float32).reshape(length, rec_heads, -1)
    values = project(recur_value).astype(jnp.float32).reshape(length, rec_heads, -1)
    inflow = (1.0 - gate_floor.reshape(rec_heads, -1)) * jax.nn.sigmoid(-forget_pre)
    decays = jnp.log1p(-inflow) - extra_decay[:, :, None]
    rec_out = recurrence(query_rows, decays, inflow, values, start_state)
    rec_rows = head_norm(rec_out, recur_gain).astype(jnp.bfloat16)
    att_heads = gate_cache.shape[1]
    att_query = project(attend_query).reshape(length, att_heads, -1)
    att_key = project(attend_key).reshape(length, att_heads, -1)
    att_value = project(attend_value).reshape(length, att_heads, -1)
    att_out = attention(att_query, att_key, att_value, gate_cache)
    att_rows = head_norm(att_out, attend_gain).astype(jnp.bfloat16)
    combined = jnp.dot(rec_rows, recur_output, preferred_element_type=jnp.float32)
    combined = combined + jnp.dot(att_rows, attend_output, preferred_element_type=jnp.float32)
    return combined.astype(jnp.bfloat16)
```

```python
import functools
import math

import jax
import jax.numpy as jnp
from jax import lax
from jax.experimental import pallas as pl
from jax.experimental.pallas import tpu as pltpu
from jax.sharding import PartitionSpec as P

FD = 64
KD = 128
EPSILON = 1e-06
BLOCK = 32
MESH = pl.DeviceIdType.MESH
F32 = jnp.float32
BF16 = jnp.bfloat16


def dot(a, b, ca=1, cb=0):
    return lax.dot_general(a, b, (((ca,), (cb,)), ((), ())), preferred_element_type=F32)


def layer_kernel(
    dims,
    tokens, gain, gate_floor, extra_decay, start_state, recur_gain, gates, attend_gain,
    w_ak, w_av, w_aq, w_rq, w_rf, w_rv, w_ro, w_ao,
    out,
    wbuf, wout, tok_all, scaled, proj, kv_all, q_all, m_ref, l_ref, acc, part, part_l,
    comb, comb_l, cum_ref, qe, rec_o, mix, st_all, chain_out, chain_in, rows_all,
    w_sem, wo_sem, tok_s, tok_r, q_s, q_r, st_s, st_r, kv_s, kv_r, ch_s, ch_r,
    po_s, po_r, pl_s, pl_r, rr_s, rr_r, ra_s, ra_r,
):
    Z, G, TP = dims
    rows, width = tokens.shape[0], recur_gain.shape[1]
    part_w = tokens.shape[1]
    model = part_w * TP
    rec_heads, att_heads = width // KD, width // FD
    c, t = lax.axis_index("sp"), lax.axis_index("tp")
    z, i = c // G, c % G

    loads = [
        pltpu.make_async_copy(w, wbuf.at[k], w_sem.at[k])
        for k, w in enumerate((w_ak, w_av, w_aq, w_rq, w_rf, w_rv))
    ]
    out_loads = [
        pltpu.make_async_copy(w, wout.at[k], wo_sem.at[k]) for k, w in enumerate((w_ro, w_ao))
    ]
    for load in loads + out_loads:
        load.start()

    barrier = pltpu.get_barrier_semaphore()
    tp_peers = [(c, (t + d) % TP) for d in range(1, TP)]
    inner_peers = [(z * G + (i + d) % G, t) for d in range(1, G)]
    outer_peers = [(((z + d) % Z) * G + i, t) for d in range(1, Z)]
    for peer in tp_peers + inner_peers + outer_peers:
        pl.semaphore_signal(barrier, inc=1, device_id=peer, device_id_type=MESH)
    pl.semaphore_wait(barrier, TP - 1 + G - 1 + Z - 1)

    def remote(src, dst, s, r, peer):
        return pltpu.make_async_remote_copy(
            src_ref=src, dst_ref=dst, send_sem=s, recv_sem=r, device_id=peer, device_id_type=MESH
        )

    tok_copies = [
        remote(tokens, tok_all.at[t], tok_s.at[d], tok_r.at[d], peer)
        for d, peer in enumerate(tp_peers)
    ]
    for copy in tok_copies:
        copy.start()
    tok_all[t] = tokens[...]
    for copy in tok_copies:
        copy.wait_recv()
    squares = jnp.zeros((rows, 1), F32)
    for p in range(TP):
        x = tok_all[p].astype(F32)
        squares = squares + jnp.sum(x * x, axis=1, keepdims=True)
        scaled[:, p * part_w:(p + 1) * part_w] = (x * gain[p]).astype(BF16)
    inverse = lax.rsqrt(squares / model + EPSILON)

    def project(k):
        return dot(scaled[...], wbuf[k]) * inverse

    loads[0].wait()
    loads[1].wait()

    def project_kv(k, carry):
        kv_all[z, k] = project(k).T.astype(BF16)
        return carry

    lax.fori_loop(0, 2, project_kv, 0)

    def kv_copy(slot):
        return remote(
            kv_all.at[slot], kv_all.at[slot], kv_s.at[slot], kv_r.at[slot], (c + G, t)
        )

    last = z == Z - 1

    @pl.when(jnp.logical_not(last))
    def _():
        kv_copy(z).start()

    loads[2].wait()
    q_all[i] = (project(2) * FD ** (-0.5)).T.astype(BF16)
    q_copies = [
        remote(q_all.at[i], q_all.at[i], q_s.at[d], q_r.at[d], peer)
        for d, peer in enumerate(inner_peers)
    ]
    for copy in q_copies:
        copy.start()
    for k in range(3, 6):
        loads[k].wait()

    def project_rec(k, carry):
        proj[k - 3] = project(k).astype(BF16)
        return carry

    lax.fori_loop(3, 6, project_rec, 0)

    rows_i = lax.broadcasted_iota(jnp.int32, (rows, rows), 0)
    cols_i = lax.broadcasted_iota(jnp.int32, (rows, rows), 1)
    lower = (cols_i <= rows_i).astype(F32).astype(BF16)
    for h in range(rec_heads):
        lanes = slice(h * KD, (h + 1) * KD)
        query = proj[0, :, lanes].astype(F32)
        value = proj[2, :, lanes]
        inflow = (1.0 - gate_floor[:, lanes]) * jax.nn.sigmoid(-proj[1, :, lanes].astype(F32))
        decay = jnp.log1p(-inflow) - extra_decay[:, h:h + 1]
        high = decay.astype(BF16)
        rest = decay - high.astype(F32)
        mid = rest.astype(BF16)
        low = (rest - mid.astype(F32)).astype(BF16)
        cum_ref[...] = dot(lower, high) + (dot(lower, mid) + dot(lower, low))
        cum = cum_ref[...]
        qe[:, lanes] = (query * jnp.exp(cum)).astype(BF16)
        end = cum[rows - 1:rows]
        key_end = (inflow * jnp.exp(end - cum)).astype(BF16)
        st_all[i, h, :KD] = dot(value, key_end, 0, 0).astype(BF16)
        st_all[i, h, KD:] = jnp.broadcast_to(jnp.exp(end), (16, KD)).astype(BF16)
        mix[...] = jnp.zeros_like(mix)
        for b in range(rows // BLOCK):
            low_r, high_r = b * BLOCK, (b + 1) * BLOCK
            middle = cum[low_r + BLOCK // 2 - 1:low_r + BLOCK // 2]
            qb = (query[low_r:high_r] * jnp.exp(cum[low_r:high_r] - middle)).astype(BF16)
            kb = (inflow[:high_r] * jnp.exp(middle - cum[:high_r])).astype(BF16)
            a = dot(qb, kb, 1, 1)
            row_at = low_r + lax.broadcasted_iota(jnp.int32, a.shape, 0)
            col_at = lax.broadcasted_iota(jnp.int32, a.shape, 1)
            mix[low_r:high_r, :high_r] = jnp.where(col_at <= row_at, a, 0.0)
        rec_o[:, lanes] = dot(mix[...].astype(BF16), value)

    st_copies = [
        remote(st_all.at[i], st_all.at[i], st_s.at[d], st_r.at[d], peer)
        for d, peer in enumerate(inner_peers)
    ]
    for copy in st_copies:
        copy.start()

    m_ref[...] = jnp.full_like(m_ref, -1e30)
    l_ref[...] = jnp.zeros_like(l_ref)
    acc[...] = jnp.zeros_like(acc)
    for copy in q_copies:
        copy.wait_recv()

    def attend(slot, j, diagonal):
        key_gates = gates[pl.ds(pl.multiple_of((slot * G + i) * rows, rows), rows), :]
        first = gates[pl.ds(pl.multiple_of((z * G + j) * rows, rows), 1), :]
        bias = first - key_gates
        if diagonal:
            allowed = i * rows + rows_i <= j * rows + cols_i
        for h in range(att_heads):
            span = slice(h * FD, (h + 1) * FD)
            s = dot(kv_all[slot, 0, span, :], q_all[j, span, :], 0, 0) + bias[:, h:h + 1]
            if diagonal:
                s = jnp.where(allowed, s, -1e30)
            before = m_ref[j, h:h + 1, :]
            top = jnp.maximum(before, jnp.max(s, axis=0, keepdims=True))
            w = jnp.exp(s - top)
            fade = jnp.exp(before - top)
            m_ref[j, h:h + 1, :] = top
            l_ref[j, h:h + 1, :] = l_ref[j, h:h + 1, :] * fade + jnp.sum(w, axis=0, keepdims=True)
            acc[j, span, :] = acc[j, span, :] * fade + dot(kv_all[slot, 1, span, :], w.astype(BF16))

    def part_copies(d):
        j = (i + d) % G
        peer = (z * G + j, t)
        return (
            remote(part.at[j], comb.at[i], po_s.at[d], po_r.at[d], peer),
            remote(part_l.at[j], comb_l.at[i], pl_s.at[d], pl_r.at[d], peer),
        )

    def finish(d):
        j = (i + d) % G
        total = jnp.maximum(l_ref[j], 1e-30)
        part_l[j] = m_ref[j] + jnp.log(total)
        for h in range(att_heads):
            span = slice(h * FD, (h + 1) * FD)
            part[j, span, :] = (acc[j, span, :] / total[h:h + 1]).astype(BF16)

        @pl.when(d < G)
        def _():
            for copy in part_copies(d):
                copy.start()

    def own_slot(d, carry):
        j = (i + d) % G

        @pl.when(j >= i)
        def _():
            attend(z, j, True)

        @pl.when(z == 0)
        def _():
            finish(d)

        return carry

    lax.fori_loop(1, G + 1, own_slot, 0)

    def earlier_slot(n, carry):
        slot = z - n
        kv_copy(slot).wait_recv()

        @pl.when(jnp.logical_not(last))
        def _():
            kv_copy(slot).start()

        def one(d, inner):
            attend(slot, (i + d) % G, False)

            @pl.when(slot == 0)
            def _():
                finish(d)

            return inner

        lax.fori_loop(1, G + 1, one, 0)
        return carry

    lax.fori_loop(1, z + 1, earlier_slot, 0)

    for copy in st_copies:
        copy.wait_recv()
    chain_copy = remote(chain_out, chain_in, ch_s, ch_r, (c + G, t))

    @pl.when(z == 0)
    def _():
        for h in range(rec_heads):
            chain_in[h] = start_state[h].T.astype(BF16)

    @pl.when(z > 0)
    def _():
        chain_copy.wait_recv()

    for h in range(rec_heads):
        lanes = slice(h * KD, (h + 1) * KD)

        def pass_on(k, state):
            return st_all[k, h, KD:KD + 1].astype(F32) * state + st_all[k, h, :KD].astype(F32)

        state = lax.fori_loop(0, i, pass_on, chain_in[h].astype(F32))
        chain_out[h] = lax.fori_loop(i, G, pass_on, state).astype(BF16)
        rec_o[:, lanes] = rec_o[:, lanes] + dot(qe[:, lanes], state.astype(BF16), 1, 1)

    @pl.when(jnp.logical_not(last))
    def _():
        chain_copy.start()

    for h in range(rec_heads):
        lanes = slice(h * KD, (h + 1) * KD)
        x = rec_o[:, lanes]
        x = x * lax.rsqrt(jnp.mean(x * x, axis=1, keepdims=True) + EPSILON)
        rows_all[0, t, :, lanes] = (x * recur_gain[:, lanes]).astype(BF16)
    row_copies = [
        [
            remote(rows_all.at[k, t], rows_all.at[k, t], s.at[d], r.at[d], peer)
            for d, peer in enumerate(tp_peers)
        ]
        for k, (s, r) in enumerate(((rr_s, rr_r), (ra_s, ra_r)))
    ]
    for copy in row_copies[0]:
        copy.start()

    comb[i] = part[i]
    comb_l[i] = part_l[i]
    for d in range(1, G):
        for copy in part_copies(d):
            copy.wait_recv()
    top = comb_l[0]
    for k in range(1, G):
        top = jnp.maximum(top, comb_l[k])
    shares = [jnp.exp(comb_l[k] - top) for k in range(G)]
    whole = shares[0]
    for k in range(1, G):
        whole = whole + shares[k]
    for h in range(att_heads):
        span = slice(h * FD, (h + 1) * FD)
        x = jnp.zeros((FD, rows), F32)
        for k in range(G):
            x = x + comb[k, span, :].astype(F32) * (shares[k][h:h + 1] / whole[h:h + 1])
        acc[0, span, :] = x * lax.rsqrt(jnp.mean(x * x, axis=0, keepdims=True) + EPSILON)
    rows_all[1, t] = (acc[0].T * attend_gain[...]).astype(BF16)
    for copy in row_copies[1]:
        copy.start()

    for load in out_loads:
        load.wait()
    for copy in row_copies[0] + row_copies[1]:
        copy.wait_recv()
    tile = min(256, out.shape[1])

    def output(n, carry):
        columns = pl.ds(pl.multiple_of(n * tile, tile), tile)
        total = jnp.zeros((rows, tile), F32)
        for k in range(2):
            for p in range(TP):
                total = total + dot(rows_all[k, p], wout[k, p * width:(p + 1) * width, columns])
        out[:, columns] = total.astype(BF16)
        return carry

    lax.fori_loop(0, out.shape[1] // tile, output, 0)

    for copy in tok_copies + q_copies + st_copies + row_copies[0] + row_copies[1]:
        copy.wait_send()
    for d in range(1, G):
        for copy in part_copies(d):
            copy.wait_send()

    @pl.when(jnp.logical_not(last))
    def _():
        chain_copy.wait_send()

        def sent(n, carry):
            kv_copy(z - n).wait_send()
            return carry

        lax.fori_loop(0, z + 1, sent, 0)


def shards(
    sizes, tokens, norm_gain, recur_query, recur_forget, recur_value, gate_floor, extra_decay,
    start_state, recur_gain, attend_query, attend_key, attend_value, gate_cache, attend_gain,
    recur_output, attend_output,
):
    sp, TP = sizes
    G = math.isqrt(sp)
    while sp % G:
        G -= 1
    Z = sp // G
    rows, part_w = tokens.shape
    width = recur_gain.shape[0]
    model = norm_gain.shape[0]
    rec_heads, att_heads = width // KD, width // FD
    out_w = recur_output.shape[1]
    vmem = pl.BlockSpec(memory_space=pltpu.VMEM)
    anywhere = pl.BlockSpec(memory_space=pl.ANY)
    dma = pltpu.SemaphoreType.DMA
    return pl.pallas_call(
        functools.partial(layer_kernel, (Z, G, TP)),
        out_shape=jax.ShapeDtypeStruct((rows, out_w), BF16),
        in_specs=[vmem] * 8 + [anywhere] * 8,
        out_specs=vmem,
        scratch_shapes=[
            pltpu.VMEM((6, model, width), BF16),
            pltpu.VMEM((2, width * TP, out_w), BF16),
            pltpu.VMEM((TP, rows, part_w), BF16),
            pltpu.VMEM((rows, model), BF16),
            pltpu.VMEM((3, rows, width), BF16),
            pltpu.VMEM((Z, 2, width, rows), BF16),
            pltpu.VMEM((G, width, rows), BF16),
            pltpu.VMEM((G, att_heads, rows), F32),
            pltpu.VMEM((G, att_heads, rows), F32),
            pltpu.VMEM((G, width, rows), F32),
            pltpu.VMEM((G, width, rows), BF16),
            pltpu.VMEM((G, att_heads, rows), F32),
            pltpu.VMEM((G, width, rows), BF16),
            pltpu.VMEM((G, att_heads, rows), F32),
            pltpu.VMEM((rows, KD), F32),
            pltpu.VMEM((rows, width), BF16),
            pltpu.VMEM((rows, width), F32),
            pltpu.VMEM((rows, rows), F32),
            pltpu.VMEM((G, rec_heads, KD + 16, KD), BF16),
            pltpu.VMEM((rec_heads, KD, KD), BF16),
            pltpu.VMEM((rec_heads, KD, KD), BF16),
            pltpu.VMEM((2, TP, rows, width), BF16),
            dma((6,)), dma((2,)),
            dma((TP,)), dma((TP,)),
            dma((G,)), dma((G,)), dma((G,)), dma((G,)),
            dma((Z,)), dma((Z,)), dma, dma,
            dma((G,)), dma((G,)), dma((G,)), dma((G,)),
            dma((TP,)), dma((TP,)), dma((TP,)), dma((TP,)),
        ],
        compiler_params=pltpu.CompilerParams(
            collective_id=0, has_side_effects=True, vmem_limit_bytes=56 * 1024 * 1024
        ),
    )(
        tokens, norm_gain.reshape(TP, 1, part_w), gate_floor.reshape(1, width), extra_decay,
        start_state, recur_gain.reshape(1, width), gate_cache, attend_gain.reshape(1, width),
        attend_key, attend_value, attend_query, recur_query, recur_forget, recur_value,
        recur_output, attend_output,
    )


def solution(mesh):
    sizes = (mesh.shape["sp"], mesh.shape["tp"])
    return jax.shard_map(
        functools.partial(shards, sizes),
        mesh=mesh,
        in_specs=(
            P("sp", "tp"),
            P(),
            P(None, "tp"),
            P(None, "tp"),
            P(None, "tp"),
            P("tp"),
            P("sp", "tp"),
            P("tp", None, None),
            P("tp"),
            P(None, "tp"),
            P(None, "tp"),
            P(None, "tp"),
            P(None, "tp"),
            P("tp"),
            P(None, "tp"),
            P(None, "tp"),
        ),
        out_specs=P("sp", "tp"),
        check_vma=False,
    )
```

```python
import functools
import math

import jax
import jax.numpy as jnp
from jax import lax
from jax.experimental import pallas as pl
from jax.experimental.pallas import tpu as pltpu
from jax.sharding import PartitionSpec as P

FD = 64
KD = 128
EPSILON = 1e-06
BLOCK = 32
MESH = pl.DeviceIdType.MESH
F32 = jnp.float32
BF16 = jnp.bfloat16


def dot(a, b, ca=1, cb=0):
    return lax.dot_general(a, b, (((ca,), (cb,)), ((), ())), preferred_element_type=F32)


def layer_kernel(
    dims,
    tokens, gain, gate_floor, extra_decay, start_state, recur_gain, gates, attend_gain,
    w_ak, w_av, w_aq, w_rq, w_rf, w_rv, w_ro, w_ao,
    out,
    wbuf, wout, tok_all, scaled, proj, kv_all, q_all, m_ref, l_ref, acc, part, part_l,
    comb, comb_l, cum_ref, qe, rec_o, mix, st_all, chain_out, chain_in, rec_all, att_all,
    out_acc, q_aug, k_aug,
    w_sem, wo_sem, tok_s, tok_r, q_s, q_r, st_s, st_r, kv_s, kv_r, ch_s, ch_r,
    po_s, po_r, pl_s, pl_r, rr_s, rr_r, ra_s, ra_r,
):
    Z, G, TP, NG = dims
    rows, width = tokens.shape[0], recur_gain.shape[1]
    part_w = tokens.shape[1]
    model = part_w * TP
    rec_heads, att_heads = width // KD, width // FD
    HG, WG = att_heads // NG, width // NG
    c, t = lax.axis_index("sp"), lax.axis_index("tp")
    z, i = c // G, c % G

    loads = [
        pltpu.make_async_copy(w, wbuf.at[k], w_sem.at[k])
        for k, w in enumerate((w_ak, w_av, w_aq, w_rq, w_rf, w_rv))
    ]
    out_loads = [
        pltpu.make_async_copy(w, wout.at[k], wo_sem.at[k]) for k, w in enumerate((w_ro, w_ao))
    ]
    for load in loads[:3]:
        load.start()

    barrier = pltpu.get_barrier_semaphore()
    tp_peers = [(c, (t + d) % TP) for d in range(1, TP)]
    inner_peers = [(z * G + (i + d) % G, t) for d in range(1, G)]
    outer_peers = [(((z + d) % Z) * G + i, t) for d in range(1, Z)]
    for peer in tp_peers + inner_peers + outer_peers:
        pl.semaphore_signal(barrier, inc=1, device_id=peer, device_id_type=MESH)
    pl.semaphore_wait(barrier, TP - 1 + G - 1 + Z - 1)

    def remote(src, dst, s, r, peer):
        return pltpu.make_async_remote_copy(
            src_ref=src, dst_ref=dst, send_sem=s, recv_sem=r, device_id=peer, device_id_type=MESH
        )

    tok_copies = [
        remote(tokens, tok_all.at[t], tok_s.at[d], tok_r.at[d], peer)
        for d, peer in enumerate(tp_peers)
    ]
    for copy in tok_copies:
        copy.start()
    for load in loads[3:] + out_loads:
        load.start()
    tok_all[t] = tokens[...]
    for copy in tok_copies:
        copy.wait_recv()
    squares = jnp.zeros((rows, 1), F32)
    for p in range(TP):
        x = tok_all[p].astype(F32)
        squares = squares + jnp.sum(x * x, axis=1, keepdims=True)
        scaled[:, p * part_w:(p + 1) * part_w] = (x * gain[p]).astype(BF16)
    inverse = lax.rsqrt(squares / model + EPSILON)

    def project(k):
        return dot(scaled[...], wbuf[k]) * inverse

    loads[2].wait()
    turned_query = (project(2) * FD ** (-0.5)).T.astype(BF16)
    for g in range(NG):
        q_all[i, g] = turned_query[g * WG:(g + 1) * WG]

    def q_copies(g):
        return [
            remote(q_all.at[i, g], q_all.at[i, g], q_s.at[d, g], q_r.at[d, g], peer)
            for d, peer in enumerate(inner_peers)
        ]

    for g in range(NG):
        for copy in q_copies(g):
            copy.start()
    loads[0].wait()
    loads[1].wait()

    def project_kv(k, carry):
        turned = project(k).T.astype(BF16)
        for g in range(NG):
            kv_all[z, g, k] = turned[g * WG:(g + 1) * WG]
        return carry

    lax.fori_loop(0, 2, project_kv, 0)

    def kv_copy(slot, g):
        ref = kv_all.at[slot, g]
        return remote(ref, ref, kv_s.at[slot, g], kv_r.at[slot, g], (c + G, t))

    last = z == Z - 1

    @pl.when(jnp.logical_not(last))
    def _():
        for g in range(NG):
            kv_copy(z, g).start()

    for k in range(3, 6):
        loads[k].wait()

    def project_rec(k, carry):
        proj[k - 3] = project(k).astype(BF16)
        return carry

    lax.fori_loop(3, 6, project_rec, 0)

    rows_i = lax.broadcasted_iota(jnp.int32, (rows, rows), 0)
    cols_i = lax.broadcasted_iota(jnp.int32, (rows, rows), 1)
    lower = (cols_i <= rows_i).astype(F32).astype(BF16)
    extra = extra_decay[...].T
    for h in range(rec_heads):
        lanes = slice(h * KD, (h + 1) * KD)
        query = proj[0, :, lanes].astype(F32)
        value = proj[2, :, lanes]
        inflow = (1.0 - gate_floor[:, lanes]) * jax.nn.sigmoid(-proj[1, :, lanes].astype(F32))
        decay = jnp.log1p(-inflow) - extra[:, h:h + 1]
        high = decay.astype(BF16)
        rest = decay - high.astype(F32)
        mid = rest.astype(BF16)
        low = (rest - mid.astype(F32)).astype(BF16)
        cum_ref[...] = dot(lower, high) + (dot(lower, mid) + dot(lower, low))
        cum = cum_ref[...]
        qe[:, lanes] = (query * jnp.exp(cum)).astype(BF16)
        end = cum[rows - 1:rows]
        key_end = (inflow * jnp.exp(end - cum)).astype(BF16)
        st_all[i, h, :KD] = dot(value, key_end, 0, 0).astype(BF16)
        st_all[i, h, KD:] = jnp.broadcast_to(jnp.exp(end), (16, KD)).astype(BF16)
        mix[...] = jnp.zeros_like(mix)
        for b in range(rows // BLOCK):
            low_r, high_r = b * BLOCK, (b + 1) * BLOCK
            middle = cum[low_r + BLOCK // 2 - 1:low_r + BLOCK // 2]
            qb = (query[low_r:high_r] * jnp.exp(cum[low_r:high_r] - middle)).astype(BF16)
            kb = (inflow[:high_r] * jnp.exp(middle - cum[:high_r])).astype(BF16)
            a = dot(qb, kb, 1, 1)
            row_at = low_r + lax.broadcasted_iota(jnp.int32, a.shape, 0)
            col_at = lax.broadcasted_iota(jnp.int32, a.shape, 1)
            mix[low_r:high_r, :high_r] = jnp.where(col_at <= row_at, a, 0.0)
        rec_o[:, lanes] = dot(mix[...].astype(BF16), value)

    st_copies = [
        remote(st_all.at[i], st_all.at[i], st_s.at[d], st_r.at[d], peer)
        for d, peer in enumerate(inner_peers)
    ]
    for copy in st_copies:
        copy.start()

    m_ref[...] = jnp.full_like(m_ref, -1e30)
    l_ref[...] = jnp.zeros_like(l_ref)
    acc[...] = jnp.zeros_like(acc)
    q_aug[:, :, FD:, :] = jnp.ones((G, att_heads, FD, rows), BF16)

    row_at = lax.broadcasted_iota(jnp.int32, (FD, rows), 0)

    def widen_queries(g, j):
        for n in range(HG):
            q_aug[j, g * HG + n, :FD, :] = q_all[j, g, n * FD:(n + 1) * FD, :]

    def widen_keys(slot, g):
        key_gates = gates[:, pl.ds(pl.multiple_of((slot * G + i) * rows, rows), rows)]
        first = gates[:, pl.ds(pl.multiple_of(z * G * rows, rows), 128)][:, :1]
        bias = first - key_gates
        for n in range(HG):
            row = bias[g * HG + n:g * HG + n + 1]
            high = row.astype(BF16).astype(F32)
            mid = (row - high).astype(BF16).astype(F32)
            low = row - high - mid
            pieces = jnp.where(row_at == 0, high, jnp.where(row_at == 1, mid, low))
            pieces = jnp.where(row_at < 3, pieces, 0.0)
            keys = kv_all[slot, g, 0, n * FD:(n + 1) * FD, :].astype(F32)
            k_aug[n] = jnp.concatenate([keys, pieces], axis=0).T.astype(BF16)

    def attend(slot, g, j, diagonal):
        for n in range(HG):
            h = g * HG + n
            span, local = slice(h * FD, (h + 1) * FD), slice(n * FD, (n + 1) * FD)
            s = dot(k_aug[n], q_aug[j, h])
            if diagonal:
                s = jnp.where(rows_i <= cols_i, s, -1e30)
            before = m_ref[j, g, n:n + 1, :]
            top = jnp.maximum(before, jnp.max(s, axis=0, keepdims=True))
            w = jnp.exp(s - top)
            fade = jnp.exp(before - top)
            m_ref[j, g, n:n + 1, :] = top
            l_ref[j, g, n:n + 1, :] = l_ref[j, g, n:n + 1, :] * fade + jnp.sum(
                w, axis=0, keepdims=True
            )
            acc[j, span, :] = acc[j, span, :] * fade + dot(
                kv_all[slot, g, 1, local, :], w.astype(BF16)
            )

    def part_copies(d, g):
        j = (i + d) % G
        peer = (z * G + j, t)
        return (
            remote(part.at[j, g], comb.at[i, g], po_s.at[d, g], po_r.at[d, g], peer),
            remote(part_l.at[j, g], comb_l.at[i, g], pl_s.at[d, g], pl_r.at[d, g], peer),
        )

    def finish(d, g):
        j = (i + d) % G
        total = jnp.maximum(l_ref[j, g], 1e-30)
        part_l[j, g] = m_ref[j, g] + jnp.log(total)
        for n in range(HG):
            h = g * HG + n
            part[j, g, n * FD:(n + 1) * FD, :] = (
                acc[j, h * FD:(h + 1) * FD, :] / total[n:n + 1]
            ).astype(BF16)

        @pl.when(d < G)
        def _():
            for copy in part_copies(d, g):
                copy.start()

    def finish_all(g):
        def one(d, carry):
            finish(d, g)
            return carry

        lax.fori_loop(1, G + 1, one, 0)

    def group(g):
        widen_queries(g, i)
        widen_keys(z, g)
        attend(z, g, i, True)
        for copy in q_copies(g):
            copy.wait_recv()
        for d in range(1, G):
            widen_queries(g, (i + d) % G)

        def own_slot(d, carry):
            j = (i + d) % G

            @pl.when(j > i)
            def _():
                attend(z, g, j, False)

            return carry

        lax.fori_loop(1, G, own_slot, 0)

        def earlier_slot(n, carry):
            slot = z - n
            kv_copy(slot, g).wait_recv()

            @pl.when(jnp.logical_not(last))
            def _():
                kv_copy(slot, g).start()

            widen_keys(slot, g)
            for j in range(G):
                attend(slot, g, j, False)
            return carry

        lax.fori_loop(1, z + 1, earlier_slot, 0)
        finish_all(g)

    def att_copies(g):
        return [
            remote(att_all.at[t, g], att_all.at[t, g], ra_s.at[d, g], ra_r.at[d, g], peer)
            for d, peer in enumerate(tp_peers)
        ]

    def combine(g):
        comb[i, g] = part[i, g]
        comb_l[i, g] = part_l[i, g]
        for d in range(1, G):
            for copy in part_copies(d, g):
                copy.wait_recv()
        top = comb_l[0, g]
        for k in range(1, G):
            top = jnp.maximum(top, comb_l[k, g])
        shares = [jnp.exp(comb_l[k, g] - top) for k in range(G)]
        whole = shares[0]
        for k in range(1, G):
            whole = whole + shares[k]
        for n in range(HG):
            span = slice(n * FD, (n + 1) * FD)
            x = jnp.zeros((FD, rows), F32)
            for k in range(G):
                x = x + comb[k, g, span, :].astype(F32) * (shares[k][n:n + 1] / whole[n:n + 1])
            acc[0, span, :] = x * lax.rsqrt(jnp.mean(x * x, axis=0, keepdims=True) + EPSILON)
        att_all[t, g] = (acc[0, :WG].T * attend_gain[:, g * WG:(g + 1) * WG]).astype(BF16)
        for copy in att_copies(g):
            copy.start()

    half = max(1, NG - 1)
    for g in range(half):
        with jax.named_scope(f"group{g}"):
            group(g)

    for copy in st_copies:
        copy.wait_recv()
    chain_copy = remote(chain_out, chain_in, ch_s, ch_r, (c + G, t))

    @pl.when(z == 0)
    def _():
        for h in range(rec_heads):
            chain_in[h] = start_state[h].T.astype(BF16)

    @pl.when(z > 0)
    def _():
        chain_copy.wait_recv()

    for h in range(rec_heads):
        lanes = slice(h * KD, (h + 1) * KD)

        def pass_on(k, state):
            return st_all[k, h, KD:KD + 1].astype(F32) * state + st_all[k, h, :KD].astype(F32)

        state = lax.fori_loop(0, i, pass_on, chain_in[h].astype(F32))
        chain_out[h] = lax.fori_loop(i, G, pass_on, state).astype(BF16)
        rec_o[:, lanes] = rec_o[:, lanes] + dot(qe[:, lanes], state.astype(BF16), 1, 1)

    @pl.when(jnp.logical_not(last))
    def _():
        chain_copy.start()

    for h in range(rec_heads):
        lanes = slice(h * KD, (h + 1) * KD)
        x = rec_o[:, lanes]
        x = x * lax.rsqrt(jnp.mean(x * x, axis=1, keepdims=True) + EPSILON)
        rec_all[t, :, lanes] = (x * recur_gain[:, lanes]).astype(BF16)
    rec_copies = [
        remote(rec_all.at[t], rec_all.at[t], rr_s.at[d], rr_r.at[d], peer)
        for d, peer in enumerate(tp_peers)
    ]
    for copy in rec_copies:
        copy.start()

    for g in range(half, NG):
        with jax.named_scope(f"group{g}"):
            group(g)

    tile = min(256, out.shape[1])

    def output(first, groups, ends):
        def columns_of(n, carry):
            columns = pl.ds(pl.multiple_of(n * tile, tile), tile)
            total = jnp.zeros((rows, tile), F32) if first else out_acc[:, columns]
            for p in range(TP):
                if first:
                    total = total + dot(rec_all[p], wout[0, p * width:(p + 1) * width, columns])
                for g in groups:
                    start = p * width + g * WG
                    total = total + dot(att_all[p, g], wout[1, start:start + WG, columns])
            if ends:
                out[:, columns] = total.astype(BF16)
            else:
                out_acc[:, columns] = total
            return carry

        lax.fori_loop(0, out.shape[1] // tile, columns_of, 0)

    with jax.named_scope("combine_a"):
        for g in range(NG - 1):
            combine(g)
        for load in out_loads:
            load.wait()
        for copy in rec_copies:
            copy.wait_recv()
        output(True, (), False)
    with jax.named_scope("combine_b"):
        combine(NG - 1)
    with jax.named_scope("last"):
        for g in range(NG):
            for copy in att_copies(g):
                copy.wait_recv()
        output(False, range(NG), True)

    for copy in tok_copies + st_copies + rec_copies:
        copy.wait_send()
    for g in range(NG):
        for copy in att_copies(g) + q_copies(g):
            copy.wait_send()
        for d in range(1, G):
            for copy in part_copies(d, g):
                copy.wait_send()

    @pl.when(jnp.logical_not(last))
    def _():
        chain_copy.wait_send()

        def sent(n, carry):
            for g in range(NG):
                kv_copy(z - n, g).wait_send()
            return carry

        lax.fori_loop(0, z + 1, sent, 0)


def shards(
    sizes, tokens, norm_gain, recur_query, recur_forget, recur_value, gate_floor, extra_decay,
    start_state, recur_gain, attend_query, attend_key, attend_value, gate_cache, attend_gain,
    recur_output, attend_output,
):
    sp, TP = sizes
    G = math.isqrt(sp)
    while sp % G:
        G -= 1
    Z = sp // G
    rows, part_w = tokens.shape
    width = recur_gain.shape[0]
    model = norm_gain.shape[0]
    rec_heads, att_heads = width // KD, width // FD
    out_w = recur_output.shape[1]
    NG = math.gcd(att_heads, 4)
    HG, WG = att_heads // NG, width // NG
    vmem = pl.BlockSpec(memory_space=pltpu.VMEM)
    anywhere = pl.BlockSpec(memory_space=pl.ANY)
    dma = pltpu.SemaphoreType.DMA
    return pl.pallas_call(
        functools.partial(layer_kernel, (Z, G, TP, NG)),
        out_shape=jax.ShapeDtypeStruct((rows, out_w), BF16),
        in_specs=[vmem] * 8 + [anywhere] * 8,
        out_specs=vmem,
        scratch_shapes=[
            pltpu.VMEM((6, model, width), BF16),
            pltpu.VMEM((2, width * TP, out_w), BF16),
            pltpu.VMEM((TP, rows, part_w), BF16),
            pltpu.VMEM((rows, model), BF16),
            pltpu.VMEM((3, rows, width), BF16),
            pltpu.VMEM((Z, NG, 2, WG, rows), BF16),
            pltpu.VMEM((G, NG, WG, rows), BF16),
            pltpu.VMEM((G, NG, HG, rows), F32),
            pltpu.VMEM((G, NG, HG, rows), F32),
            pltpu.VMEM((G, width, rows), F32),
            pltpu.VMEM((G, NG, WG, rows), BF16),
            pltpu.VMEM((G, NG, HG, rows), F32),
            pltpu.VMEM((G, NG, WG, rows), BF16),
            pltpu.VMEM((G, NG, HG, rows), F32),
            pltpu.VMEM((rows, KD), F32),
            pltpu.VMEM((rows, width), BF16),
            pltpu.VMEM((rows, width), F32),
            pltpu.VMEM((rows, rows), F32),
            pltpu.VMEM((G, rec_heads, KD + 16, KD), BF16),
            pltpu.VMEM((rec_heads, KD, KD), BF16),
            pltpu.VMEM((rec_heads, KD, KD), BF16),
            pltpu.VMEM((TP, rows, width), BF16),
            pltpu.VMEM((TP, NG, rows, WG), BF16),
            pltpu.VMEM((rows, out_w), F32),
            pltpu.VMEM((G, att_heads, 2 * FD, rows), BF16),
            pltpu.VMEM((HG, rows, 2 * FD), BF16),
            dma((6,)), dma((2,)),
            dma((TP,)), dma((TP,)),
            dma((G, NG)), dma((G, NG)), dma((G,)), dma((G,)),
            dma((Z, NG)), dma((Z, NG)), dma, dma,
            dma((G, NG)), dma((G, NG)), dma((G, NG)), dma((G, NG)),
            dma((TP,)), dma((TP,)), dma((TP, NG)), dma((TP, NG)),
        ],
        compiler_params=pltpu.CompilerParams(
            collective_id=0, has_side_effects=True, vmem_limit_bytes=56 * 1024 * 1024
        ),
    )(
        tokens, norm_gain.reshape(TP, 1, part_w), gate_floor.reshape(1, width), extra_decay.T,
        start_state, recur_gain.reshape(1, width), gate_cache.T, attend_gain.reshape(1, width),
        attend_key, attend_value, attend_query, recur_query, recur_forget, recur_value,
        recur_output, attend_output,
    )


def solution(mesh):
    sizes = (mesh.shape["sp"], mesh.shape["tp"])
    return jax.shard_map(
        functools.partial(shards, sizes),
        mesh=mesh,
        in_specs=(
            P("sp", "tp"),
            P(),
            P(None, "tp"),
            P(None, "tp"),
            P(None, "tp"),
            P("tp"),
            P("sp", "tp"),
            P("tp", None, None),
            P("tp"),
            P(None, "tp"),
            P(None, "tp"),
            P(None, "tp"),
            P(None, "tp"),
            P("tp"),
            P(None, "tp"),
            P(None, "tp"),
        ),
        out_specs=P("sp", "tp"),
        check_vma=False,
    )
```
